32 devices in a mesh: tp: 16 (over z, y, x), dp: 2 (over core).
Axes of the slice: x: 2, y: 2, z: 4, core: 2. Of those that a mesh axis runs over, the one named last changes fastest.
Arguments:
- hidden: bfloat16 [16, 4096], P(None, 'dp'), may hold values from -6 to 6
- norm_gain: float32 [2, 4096], P(None, 'dp'), may hold values from 0.1 to 1.9
- gate_weight: bfloat16 [2, 4096, 8192], P(None, 'dp', 'tp'), may hold values from -0.09375 to 0.09375
- inner_weight: bfloat16 [2, 4096, 8192], P(None, 'dp', 'tp'), may hold values from -0.09375 to 0.09375
- write_weight: bfloat16 [2, 4096, 2048], P(None, 'dp', 'tp'), may hold values from -0.09375 to 0.09375
- read_weight: bfloat16 [2, 4096, 2048], P(None, 'dp', 'tp'), may hold values from -0.09375 to 0.09375
- step_weight: bfloat16 [2, 4096, 128], P(None, 'dp'), may hold values from -0.09375 to 0.09375
- conv_inner: bfloat16 [2, 4, 8192], P(None, None, 'tp'), may hold values from -3 to 3
- conv_write: bfloat16 [2, 4, 2048], P(None, None, 'tp'), may hold values from -3 to 3
- conv_read: bfloat16 [2, 4, 2048], P(None, None, 'tp'), may hold values from -3 to 3
- step_bias: float32 [2, 128], P(None, 'tp'), may hold values from -4 to -1
- decay_log: float32 [2, 128], P(None, 'tp'), may hold values from -3 to 0.5
- skip_gain: float32 [2, 128], P(None, 'tp'), may hold values from 0.1 to 1.9
- group_gain: float32 [2, 8192], P(None, 'tp'), may hold values from 0.1 to 1.9
- out_weight: bfloat16 [2, 8192, 4096], P(None, 'tp', 'dp'), may hold values from -0.4 to 0.4
- state_inner: bfloat16 [2, 16, 3, 8192], P(None, 'dp', None, 'tp'), may hold values from -6 to 6
- state_write: bfloat16 [2, 16, 3, 2048], P(None, 'dp', None, 'tp'), may hold values from -6 to 6
- state_read: bfloat16 [2, 16, 3, 2048], P(None, 'dp', None, 'tp'), may hold values from -6 to 6
- recurrent: float32 [2, 16, 128, 64, 128], P(None, 'dp', 'tp'), may hold values from -1.2 to 1.2, as said below
Outputs:
- out_hidden: bfloat16 [16, 4096], P(None, 'dp')
- next_inner: bfloat16 [2, 16, 3, 8192], P(None, 'dp', None, 'tp')
- next_write: bfloat16 [2, 16, 3, 2048], P(None, 'dp', None, 'tp')
- next_read: bfloat16 [2, 16, 3, 2048], P(None, 'dp', None, 'tp')
- next_recurrent: float32 [2, 16, 128, 64, 128], P(None, 'dp', 'tp')
The draws below stay inside these ranges and needn't reach their ends.
Inputs may be any that keep to these rules, and one draw needn't show every extreme that they name: recurrent states of order a tenth, with scales that differ between heads.
All inputs are finite; a program needn't handle non-finite values.
Results may differ from the reference program's by a relative error of at most 0.025.
Values may be sent and summed in bfloat16 or wider, within the bound.
A program may use at most 64 MiB of HBM per device.

```python
import math
import jax
import jax.numpy as jnp
from jax import lax

D = 4096
HEADS = 128
HEAD_DIM = 64
STATE_DIM = 128
GROUPS = 16
KERNEL = 4
LAYERS = 2
INNER = 8192
BATCH = 16
N_DP = 2


def draw_recurrent(key, part):
    first_key, second_key = jax.random.split(jax.random.fold_in(key, 17))
    shape = (LAYERS, BATCH, HEADS, HEAD_DIM, STATE_DIM)
    factor = jnp.exp(jax.random.uniform(first_key, (LAYERS, 1, HEADS, 1, 1), jnp.float32, math.log(0.03), math.log(0.3)))
    values = jax.random.truncated_normal(second_key, -4.0, 4.0, shape, jnp.float32)
    return (values * factor).astype(jnp.float32)


def draw_out_weight(key, part):
    sign_key, size_key, common_key, noise_key = jax.random.split(jax.random.fold_in(key, 29), 4)
    shape = (LAYERS, INNER, D)
    signs = jnp.where(jax.random.bernoulli(sign_key, 0.5, (LAYERS, INNER, 1)), 1.0, -1.0).astype(jnp.float32)
    magnitude = jax.random.uniform(size_key, (LAYERS, INNER, 1), jnp.float32, 1.0, 1.3)
    common = jax.random.truncated_normal(common_key, -4.0, 4.0, (LAYERS, 1, D), jnp.float32)
    noise = jax.random.truncated_normal(noise_key, -4.0, 4.0, shape, jnp.float32)
    values = (signs * magnitude * common + noise) / math.sqrt(INNER)
    return values.astype(jnp.bfloat16)


def shard_levels(stream_key, shape, cuts, smallest, high):
    def one(dim, parts):
        heights = jax.random.uniform(jax.random.fold_in(jax.random.fold_in(stream_key, 6), dim), (parts,), jnp.float32, smallest / len(cuts), high / len(cuts))
        return jnp.repeat(jnp.exp(heights), shape[dim] // parts).reshape((-1,) + (1,) * (len(shape) - dim - 1))

    factor_of = one(*cuts[0])
    for cut in cuts[1:]:
        factor_of = factor_of * one(*cut)
    return factor_of


def gaussian(key, extent, spread, reach, cuts=(), dtype=jnp.bfloat16):
    gain = shard_levels(key, extent, cuts, -0.22, 0.18) if cuts else 1.0
    drawn = jax.random.normal(key, extent, jnp.float32) * spread * gain
    return jnp.minimum(jnp.maximum(drawn, -reach), reach).astype(dtype)


def setup_inputs(seed: int = 0) -> dict:
    streams_of = jax.random.split(jax.random.key(seed), 20)
    return {
        "hidden": gaussian(streams_of[0], (BATCH, D), 1.0, 6.0, ((1, 2),)),
        "norm_gain": jnp.clip(1.0 + 0.18 * jax.random.normal(streams_of[1], (LAYERS, D), jnp.float32), 0.1, 1.9),
        "gate_weight": gaussian(streams_of[2], (LAYERS, D, INNER), D ** -0.5, 0.09375, ((1, 2), (2, 16))),
        "inner_weight": gaussian(streams_of[3], (LAYERS, D, INNER), D ** -0.5, 0.09375, ((1, 2), (2, 16))),
        "write_weight": gaussian(streams_of[4], (LAYERS, D, GROUPS * STATE_DIM), D ** -0.5, 0.09375, ((1, 2), (2, 16))),
        "read_weight": gaussian(streams_of[5], (LAYERS, D, GROUPS * STATE_DIM), D ** -0.5, 0.09375, ((1, 2), (2, 16))),
        "step_weight": gaussian(streams_of[6], (LAYERS, D, HEADS), D ** -0.5, 0.09375, ((1, 2),)),
        "conv_inner": gaussian(streams_of[7], (LAYERS, KERNEL, INNER), KERNEL ** -0.5, 3.0, ((2, 16),)),
        "conv_write": gaussian(streams_of[8], (LAYERS, KERNEL, GROUPS * STATE_DIM), KERNEL ** -0.5, 3.0, ((2, 16),)),
        "conv_read": gaussian(streams_of[9], (LAYERS, KERNEL, GROUPS * STATE_DIM), KERNEL ** -0.5, 3.0, ((2, 16),)),
        "step_bias": jnp.clip(-4.0 + 3.0 * jax.random.uniform(streams_of[10], (LAYERS, HEADS), jnp.float32) ** shard_levels(streams_of[10], (LAYERS, HEADS), ((1, 16),), -0.2, 0.2), -4.0, -1.0),
        "decay_log": jnp.clip(-3.0 + 3.5 * jax.random.uniform(streams_of[11], (LAYERS, HEADS), jnp.float32) ** shard_levels(streams_of[11], (LAYERS, HEADS), ((1, 16),), -0.2, 0.2), -3.0, 0.5),
        "skip_gain": jnp.clip(1.0 + 0.18 * jax.random.normal(streams_of[12], (LAYERS, HEADS), jnp.float32), 0.1, 1.9),
        "group_gain": jnp.clip(1.0 + 0.18 * jax.random.normal(streams_of[13], (LAYERS, INNER), jnp.float32), 0.1, 1.9),
        "out_weight": draw_out_weight(jax.random.fold_in(streams_of[19], 71), 0),
        "state_inner": gaussian(streams_of[15], (LAYERS, BATCH, KERNEL - 1, INNER), 1.0, 6.0, ((1, 2), (3, 16))),
        "state_write": gaussian(streams_of[16], (LAYERS, BATCH, KERNEL - 1, GROUPS * STATE_DIM), 1.0, 6.0, ((1, 2), (3, 16))),
        "state_read": gaussian(streams_of[17], (LAYERS, BATCH, KERNEL - 1, GROUPS * STATE_DIM), 1.0, 6.0, ((1, 2), (3, 16))),
        "recurrent": draw_recurrent(jax.random.fold_in(streams_of[19], 71), 0),
    }


eps = 1e-06

def project(normed, weight):
    block_rows = D // N_DP
    left_side = normed.reshape(normed.shape[0], N_DP, block_rows).astype(jnp.float32)
    right_side = weight.reshape(N_DP, block_rows, weight.shape[1]).astype(jnp.float32)
    pieces = jnp.einsum('bkr,krc->kbc', left_side, right_side)
    pieces = lax.optimization_barrier(pieces.astype(jnp.bfloat16)).astype(jnp.float32)
    return lax.optimization_barrier(jnp.sum(pieces, axis=0)).astype(jnp.bfloat16)

def convolve(state, fresh_row, kernel):
    window = jnp.concatenate([state, fresh_row[:, None, :]], axis=1)
    summed = lax.optimization_barrier(jnp.sum(window.astype(jnp.float32) * kernel.astype(jnp.float32)[None], axis=1))
    return (jax.nn.silu(summed), window[:, 1:])

def mixer_block(stream, number, norm_gain, gate_weight, inner_weight, write_weight, read_weight, step_weight, conv_inner, conv_write, conv_read, step_bias, decay_log, skip_gain, group_gain, out_weight, state_inner, state_write, state_read, recurrent):
    wide_in = stream.astype(jnp.float32)
    factor = lax.rsqrt(lax.optimization_barrier(jnp.mean(wide_in * wide_in, axis=1, keepdims=True)) + eps)
    normed = (wide_in * factor * norm_gain[number][None, :]).astype(jnp.bfloat16)
    gate_raw = project(normed, gate_weight[number])
    inner_raw = project(normed, inner_weight[number])
    write_raw = project(normed, write_weight[number])
    read_raw = project(normed, read_weight[number])
    step_raw = project(normed, step_weight[number])
    inner_act, next_inner = convolve(state_inner[number], inner_raw, conv_inner[number])
    write_act, next_write = convolve(state_write[number], write_raw, conv_write[number])
    read_act, next_read = convolve(state_read[number], read_raw, conv_read[number])
    write_act = write_act.astype(jnp.bfloat16)
    read_act = read_act.astype(jnp.bfloat16)
    rows_here = stream.shape[0]
    per_group = HEADS // GROUPS
    write_groups = jnp.transpose(write_act.reshape(rows_here, STATE_DIM, GROUPS), (0, 2, 1))
    read_groups = jnp.transpose(read_act.reshape(rows_here, STATE_DIM, GROUPS), (0, 2, 1))
    write_vec = jnp.repeat(write_groups, per_group, axis=1).astype(jnp.float32)
    read_vec = jnp.repeat(read_groups, per_group, axis=1).astype(jnp.float32)
    step_size = jax.nn.softplus(step_raw.astype(jnp.float32) + step_bias[number][None, :])
    retain = jnp.exp(-step_size * jnp.exp(decay_log[number])[None, :])
    inner_heads = inner_act.reshape(rows_here, HEADS, HEAD_DIM)
    updated = retain[:, :, None, None] * recurrent[number] + (step_size[:, :, None] * inner_heads)[:, :, :, None] * write_vec[:, :, None, :]
    readout = jnp.einsum('bhpn,bhn->bhp', updated, read_vec, precision=lax.Precision.HIGHEST)
    readout = readout + skip_gain[number][None, :, None] * inner_heads
    gated_out = readout.reshape(rows_here, INNER) * jax.nn.silu(gate_raw.astype(jnp.float32))
    grouped = gated_out.reshape(rows_here, GROUPS, INNER // GROUPS)
    group_factor = lax.rsqrt(lax.optimization_barrier(jnp.mean(grouped * grouped, axis=2, keepdims=True)) + eps)
    group_normed = ((grouped * group_factor).reshape(rows_here, INNER) * group_gain[number][None, :]).astype(jnp.bfloat16)
    branch = jnp.dot(group_normed, out_weight[number], preferred_element_type=jnp.float32)
    result = (wide_in + branch).astype(jnp.bfloat16)
    return (result, next_inner, next_write, next_read, updated)

def reference(hidden, norm_gain, gate_weight, inner_weight, write_weight, read_weight, step_weight, conv_inner, conv_write, conv_read, step_bias, decay_log, skip_gain, group_gain, out_weight, state_inner, state_write, state_read, recurrent):
    stream = hidden
    collected = [[], [], [], []]
    for number in range(LAYERS):
        outcome = mixer_block(stream, number, norm_gain, gate_weight, inner_weight, write_weight, read_weight, step_weight, conv_inner, conv_write, conv_read, step_bias, decay_log, skip_gain, group_gain, out_weight, state_inner, state_write, state_read, recurrent)
        stream = outcome[0]
        for position in range(4):
            collected[position].append(outcome[position + 1])
    return (stream, jnp.stack(collected[0]), jnp.stack(collected[1]), jnp.stack(collected[2]), jnp.stack(collected[3]))
```

```python
import jax
import jax.numpy as jnp
from jax import lax
from jax.experimental import pallas as pl
from jax.experimental.pallas import tpu as pltpu
from jax.sharding import PartitionSpec as P

D = 4096
HEADS = 128
GROUPS = 16


eps = 1e-06


def convolve(state, fresh_row, kernel):
    window = jnp.concatenate([state, fresh_row[:, None, :]], axis=1)
    summed = jnp.sum(window.astype(jnp.float32) * kernel.astype(jnp.float32)[None], axis=1)
    return (jax.nn.silu(summed), window[:, 1:])


def mixer_block(normed, number, weights):
    (
        gate_weight,
        inner_weight,
        write_weight,
        read_weight,
        step_weight,
        conv_inner,
        conv_write,
        conv_read,
        step_bias,
        decay_log,
        skip_gain,
        group_gain,
        out_weight,
        state_inner,
        state_write,
        state_read,
        recurrent,
    ) = weights

    def partial_of(weight):
        return jnp.dot(normed, weight[number], preferred_element_type=jnp.float32).astype(
            jnp.bfloat16
        )

    summed = (
        lax.psum_scatter(partial_of(gate_weight), "dp", scatter_dimension=0, tiled=True).astype(
            jnp.float32
        ),
        lax.psum_scatter(partial_of(inner_weight), "dp", scatter_dimension=0, tiled=True).astype(
            jnp.float32
        ),
        lax.psum_scatter(partial_of(write_weight), "dp", scatter_dimension=0, tiled=True).astype(
            jnp.float32
        ),
        lax.psum_scatter(partial_of(read_weight), "dp", scatter_dimension=0, tiled=True).astype(
            jnp.float32
        ),
        lax.psum_scatter(partial_of(step_weight), "dp", scatter_dimension=0, tiled=True).astype(
            jnp.float32
        ),
    )
    gate_raw, inner_raw, write_raw, read_raw, step_raw = [
        member.astype(jnp.bfloat16) for member in summed
    ]
    inner_act, next_inner = convolve(state_inner[number], inner_raw, conv_inner[number])
    write_act, next_write = convolve(state_write[number], write_raw, conv_write[number])
    read_act, next_read = convolve(state_read[number], read_raw, conv_read[number])
    write_all, read_all = (
        lax.all_gather(write_act.astype(jnp.bfloat16), "tp", axis=1, tiled=True),
        lax.all_gather(read_act.astype(jnp.bfloat16), "tp", axis=1, tiled=True),
    )
    heads_here = step_bias.shape[1]
    head_dim = recurrent.shape[3]
    state_dim = recurrent.shape[4]
    rows_here = inner_act.shape[0]
    first_head = lax.axis_index("tp") * heads_here
    group_index = first_head // (HEADS // GROUPS)
    write_grid = write_all.reshape(rows_here, state_dim, GROUPS)
    read_grid = read_all.reshape(rows_here, state_dim, GROUPS)
    write_vec = lax.dynamic_slice_in_dim(write_grid, group_index, 1, 2)[:, :, 0].astype(jnp.float32)
    read_vec = lax.dynamic_slice_in_dim(read_grid, group_index, 1, 2)[:, :, 0].astype(jnp.float32)
    step_own = lax.dynamic_slice_in_dim(step_raw, first_head, heads_here, 1)
    step_size = jax.nn.softplus(step_own.astype(jnp.float32) + step_bias[number][None, :])
    retain = jnp.exp(-step_size * jnp.exp(decay_log[number])[None, :])
    inner_heads = inner_act.reshape(rows_here, heads_here, head_dim)
    updated = (
        retain[:, :, None, None] * recurrent[number]
        + (step_size[:, :, None] * inner_heads)[:, :, :, None] * write_vec[:, None, None, :]
    )
    readout = jnp.einsum("bhpn,bn->bhp", updated, read_vec, precision=lax.Precision.HIGHEST)
    readout = readout + skip_gain[number][None, :, None] * inner_heads
    gated_out = readout.reshape(rows_here, heads_here * head_dim) * jax.nn.silu(
        gate_raw.astype(jnp.float32)
    )
    selector = (jnp.arange(GROUPS) == group_index).astype(jnp.float32)
    totals = lax.psum(jnp.sum(gated_out * gated_out, axis=1)[:, None] * selector[None, :], "tp")
    group_sum = jnp.sum(totals * selector[None, :], axis=1, keepdims=True)
    group_factor = lax.rsqrt(group_sum / (HEADS // GROUPS * head_dim) + eps)
    group_normed = (gated_out * group_factor * group_gain[number][None, :]).astype(jnp.bfloat16)
    branch = jnp.dot(
        lax.all_gather(group_normed, "dp", axis=0, tiled=True),
        out_weight[number],
        preferred_element_type=jnp.float32,
    )
    return (branch, (next_inner, next_write, next_read, updated))


def total_over(branch):
    return lax.psum(branch, "tp")


def local(
    hidden,
    norm_gain,
    gate_weight,
    inner_weight,
    write_weight,
    read_weight,
    step_weight,
    conv_inner,
    conv_write,
    conv_read,
    step_bias,
    decay_log,
    skip_gain,
    group_gain,
    out_weight,
    state_inner,
    state_write,
    state_read,
    recurrent,
):
    weights = (
        gate_weight,
        inner_weight,
        write_weight,
        read_weight,
        step_weight,
        conv_inner,
        conv_write,
        conv_read,
        step_bias,
        decay_log,
        skip_gain,
        group_gain,
        out_weight,
        state_inner,
        state_write,
        state_read,
        recurrent,
    )
    wide_in = hidden.astype(jnp.float32)
    squares = lax.psum(jnp.sum(wide_in * wide_in, axis=1, keepdims=True), "dp")
    normed = (wide_in * lax.rsqrt(squares / D + eps) * norm_gain[0][None, :]).astype(jnp.bfloat16)
    branch, first_states = mixer_block(normed, 0, weights)
    middle = (wide_in + total_over(branch)).astype(jnp.bfloat16).astype(jnp.float32)
    squares = lax.psum(jnp.sum(middle * middle, axis=1, keepdims=True), "dp")
    normed = (middle * lax.rsqrt(squares / D + eps) * norm_gain[1][None, :]).astype(jnp.bfloat16)
    branch, second_states = mixer_block(normed, 1, weights)
    result = (middle + total_over(branch)).astype(jnp.bfloat16)
    stacked = [jnp.stack([earlier, later]) for earlier, later in zip(first_states, second_states)]
    return (result, stacked[0], stacked[1], stacked[2], stacked[3])


def fused_kernel(
    tp,
    hidden_ref,
    norm_gain_ref,
    tap_ref,
    pre_ref,
    bias_ref,
    decay_ref,
    skip_ref,
    group_gain_ref,
    gate_hbm,
    inner_hbm,
    write_hbm,
    read_hbm,
    step_hbm,
    out_hbm,
    rec_hbm,
    result_ref,
    raw_ref,
    retain_ref,
    scaled_ref,
    vec_ref,
    gate_v,
    inner_v,
    small_v,
    out_v,
    rec_v,
    pick_v,
    spread_v,
    part_a,
    part_b,
    got_a,
    got_b,
    gath,
    normed_mine,
    normed_peer,
    branch_v,
    red,
    stream_v,
    w_sem,
    dp_send,
    dp_recv,
    gath_send,
    gath_recv,
    red_send,
    red_recv,
    str_send,
    str_recv,
):
    t = lax.axis_index("tp")
    me = lax.axis_index("dp")
    peer = 1 - me
    layers = norm_gain_ref.shape[0]
    rows = hidden_ref.shape[0]
    own = rows // 2
    width = hidden_ref.shape[1]
    total_width = width * 2
    inner = gate_hbm.shape[2]
    cols = write_hbm.shape[2]
    step_cols = step_hbm.shape[2]
    small = 2 * cols + step_cols
    chunk = width // tp
    heads = bias_ref.shape[1]
    head_dim = inner // heads

    def load(source, target, number):
        return pltpu.make_async_copy(source, target, w_sem.at[number])

    loads = []
    for l in range(layers):
        at = 7 * l
        loads.append(
            [
                load(write_hbm.at[l], small_v.at[l, :, pl.ds(0, cols)], at),
                load(read_hbm.at[l], small_v.at[l, :, pl.ds(cols, cols)], at + 1),
                load(step_hbm.at[l], small_v.at[l, :, pl.ds(2 * cols, step_cols)], at + 2),
                load(inner_hbm.at[l], inner_v.at[l], at + 3),
                load(gate_hbm.at[l], gate_v.at[l], at + 4),
                load(rec_hbm.at[l], rec_v.at[l], at + 5),
                load(out_hbm.at[l], out_v.at[l], at + 6),
            ]
        )
    for l in range(layers):
        for one in loads[l]:
            one.start()

    barrier = pltpu.get_barrier_semaphore()

    @pl.loop(1, tp)
    def _(k):
        pl.semaphore_signal(barrier, inc=1, device_id={"tp": lax.rem(t + k, tp), "dp": me})

    pl.semaphore_signal(barrier, inc=1, device_id={"tp": t, "dp": peer})

    big = pick_v.shape
    pick_v[...] = (
        lax.broadcasted_iota(jnp.int32, big, 0)
        == lax.broadcasted_iota(jnp.int32, big, 1) * tp + t
    ).astype(jnp.float32).astype(jnp.bfloat16)
    grid = spread_v.shape
    lane_head = lax.broadcasted_iota(jnp.int32, grid, 1) // head_dim
    spread_v[...] = (
        lax.broadcasted_iota(jnp.int32, grid, 0) == lane_head + heads * t
    ).astype(jnp.float32).astype(jnp.bfloat16)

    wide_head = lax.broadcasted_iota(jnp.int32, (own, inner), 1) // head_dim
    own_row = lax.broadcasted_iota(jnp.int32, (own, inner), 0)

    def widen(row):
        wide = jnp.zeros((own, inner), jnp.float32)
        for h in range(heads):
            wide = jnp.where(
                wide_head == h, jnp.broadcast_to(row[:, h : h + 1], (own, inner)), wide
            )
        return wide

    bias_w = [widen(bias_ref[l : l + 1, :]) for l in range(layers)]
    rate_w = [widen(jnp.exp(decay_ref[l : l + 1, :])) for l in range(layers)]
    skip_w = [widen(skip_ref[l : l + 1, :]) for l in range(layers)]

    def to_peer(source, target, number):
        return pltpu.make_async_remote_copy(
            src_ref=source,
            dst_ref=target,
            send_sem=dp_send.at[number],
            recv_sem=dp_recv.at[number],
            device_id={"tp": t, "dp": peer},
        )

    def spread_start(source_of, target, sends, recvs):
        @pl.loop(1, tp)
        def _(k):
            to = lax.rem(t + k, tp)
            pltpu.make_async_remote_copy(
                src_ref=source_of(to),
                dst_ref=target.at[t],
                send_sem=sends.at[to],
                recv_sem=recvs.at[t],
                device_id={"tp": to, "dp": me},
            ).start()

    def spread_wait(source_of, target, sends, recvs):
        @pl.loop(1, tp)
        def _(k):
            to = lax.rem(t + k, tp)
            copy = pltpu.make_async_remote_copy(
                src_ref=source_of(to),
                dst_ref=target.at[to],
                send_sem=sends.at[to],
                recv_sem=recvs.at[to],
                device_id={"tp": to, "dp": me},
            )
            copy.wait_send()
            copy.wait_recv()

    first = True
    mine = pl.ds(pl.multiple_of(me * own, own), own)
    theirs = pl.ds(pl.multiple_of(peer * own, own), own)
    wide = hidden_ref[...].astype(jnp.float32)
    for l in range(layers):
        scaled = (wide * norm_gain_ref[l : l + 1, :]).astype(jnp.bfloat16)
        squares = jnp.sum(wide * wide, axis=1, keepdims=True)
        for one in loads[l][:3]:
            one.wait()
        part_a[l, :, 0:small] = jnp.dot(scaled, small_v[l], preferred_element_type=jnp.float32)
        part_a[l, :, small : small + 128] = jnp.broadcast_to(squares, (rows, 128))
        if first:
            pl.semaphore_wait(barrier, tp)
            first = False
        send_a = to_peer(part_a.at[l, theirs], got_a.at[l], 3 * l)
        send_a.start()
        loads[l][3].wait()
        part_b[l, :, 0:inner] = jnp.dot(scaled, inner_v[l], preferred_element_type=jnp.float32)
        loads[l][4].wait()
        part_b[l, :, inner : 2 * inner] = jnp.dot(
            scaled, gate_v[l], preferred_element_type=jnp.float32
        )
        send_b = to_peer(part_b.at[l, theirs], got_b.at[l], 3 * l + 1)
        send_b.start()
        send_a.wait()
        sum_a = part_a[l, mine, :] + got_a[l]
        factor = lax.rsqrt(sum_a[:, small : small + 1] / total_width + eps)
        raw_a = (sum_a[:, 0:small] * factor).astype(jnp.bfloat16).astype(jnp.float32)
        raw_ref[l, :, inner : inner + 2 * cols] = raw_a[:, 0 : 2 * cols]
        tapped = (
            pre_ref[l, :, inner : inner + 2 * cols]
            + raw_a[:, 0 : 2 * cols] * tap_ref[l : l + 1, inner : inner + 2 * cols]
        )
        tapped = tapped * jax.nn.sigmoid(tapped)
        gath[l, t] = jnp.concatenate([tapped[:, :cols], tapped[:, cols:]], axis=0).astype(
            jnp.bfloat16
        )
        spread_start(lambda to: gath.at[l, t], gath.at[l], gath_send.at[l], gath_recv.at[l])
        step_raw = raw_a[:, 2 * cols :]
        step = (
            jnp.dot(
                jnp.concatenate([step_raw, step_raw], axis=0).astype(jnp.bfloat16),
                spread_v[...],
                preferred_element_type=jnp.float32,
            )[:own]
            + bias_w[l]
        )
        step = jnp.maximum(step, 0.0) + jnp.log1p(jnp.exp(-jnp.abs(step)))
        retain = jnp.exp(-step * rate_w[l])
        retain_ref[l] = retain
        send_b.wait()
        raw_b = (
            ((part_b[l, mine, :] + got_b[l]) * factor).astype(jnp.bfloat16).astype(jnp.float32)
        )
        raw_ref[l, :, 0:inner] = raw_b[:, 0:inner]
        act = pre_ref[l, :, 0:inner] + raw_b[:, 0:inner] * tap_ref[l : l + 1, 0:inner]
        act = act * jax.nn.sigmoid(act)
        gate = raw_b[:, inner:]
        gate = gate * jax.nn.sigmoid(gate)
        grown = step * act
        scaled_ref[l] = grown
        loads[l][5].wait()
        spread_wait(lambda to: gath.at[l, t], gath.at[l], gath_send.at[l], gath_recv.at[l])
        both = jnp.dot(
            jnp.concatenate([gath[l, k] for k in range(tp)], axis=1),
            pick_v[...],
            preferred_element_type=jnp.float32,
        )
        vec_ref[l] = both[:own]
        overlap = jnp.sum(both[:own] * both[own:], axis=1, keepdims=True)
        low = both.astype(jnp.bfloat16)
        carried = jnp.zeros((own, inner), jnp.float32)
        for b in range(own):
            held = rec_v[l, b].reshape(inner, rec_v.shape[-1]).astype(jnp.bfloat16)
            row = lax.dot_general(
                low, held, (((1,), (1,)), ((), ())), preferred_element_type=jnp.float32
            )
            carried = jnp.where(own_row == b, row[own:], carried)
        gated = (retain * carried + grown * overlap + skip_w[l] * act) * gate
        group = jnp.sum(gated * gated, axis=1, keepdims=True) / inner
        normed = gated * lax.rsqrt(group + eps) * group_gain_ref[l : l + 1, :]
        normed_mine[l] = normed
        send_c = to_peer(normed_mine.at[l], normed_peer.at[l], 3 * l + 2)
        send_c.start()
        loads[l][6].wait()
        send_c.wait()
        other = normed_peer[l]
        lower = me == 0
        left = jnp.concatenate(
            [jnp.where(lower, normed, other), jnp.where(lower, other, normed)], axis=0
        ).astype(jnp.bfloat16)
        branch = jnp.dot(left, out_v[l], preferred_element_type=jnp.float32).astype(jnp.bfloat16)
        for k in range(tp):
            branch_v[l, k] = branch[:, k * chunk : (k + 1) * chunk]
        spread_start(lambda to: branch_v.at[l, to], red.at[l], red_send.at[l], red_recv.at[l])
        red[l, t] = branch_v[l, t]
        spread_wait(lambda to: branch_v.at[l, to], red.at[l], red_send.at[l], red_recv.at[l])
        total = red[l, 0].astype(jnp.float32)
        for k in range(1, tp):
            total = total + red[l, k].astype(jnp.float32)
        if l == 0:
            before = hidden_ref[:, pl.ds(pl.multiple_of(t * chunk, chunk), chunk)]
        else:
            before = stream_v[l - 1, t]
        stream_v[l, t] = (total + before.astype(jnp.float32)).astype(jnp.bfloat16)
        spread_start(lambda to: stream_v.at[l, t], stream_v.at[l], str_send.at[l], str_recv.at[l])
        spread_wait(lambda to: stream_v.at[l, t], stream_v.at[l], str_send.at[l], str_recv.at[l])
        after = jnp.concatenate([stream_v[l, k] for k in range(tp)], axis=1)
        if l == layers - 1:
            result_ref[...] = after
        else:
            wide = after.astype(jnp.float32)


def fused_local(
    hidden,
    norm_gain,
    gate_weight,
    inner_weight,
    write_weight,
    read_weight,
    step_weight,
    conv_inner,
    conv_write,
    conv_read,
    step_bias,
    decay_log,
    skip_gain,
    group_gain,
    out_weight,
    state_inner,
    state_write,
    state_read,
    recurrent,
):
    tp = lax.axis_size("tp")
    layers, width, inner = gate_weight.shape
    cols = write_weight.shape[2]
    step_cols = step_weight.shape[2]
    rows = hidden.shape[0]
    own, heads, head_dim, state_dim = recurrent.shape[1:]
    chunk = width // tp
    taps = jnp.concatenate([conv_inner, conv_write, conv_read], axis=2).astype(jnp.float32)
    held = jnp.concatenate([state_inner, state_write, state_read], axis=3).astype(jnp.float32)
    pre = jnp.sum(held * taps[:, None, :-1], axis=2)
    vmem = pl.BlockSpec(memory_space=pltpu.VMEM)
    hbm = pl.BlockSpec(memory_space=pl.ANY)
    f32, bf16 = jnp.float32, jnp.bfloat16
    dma = pltpu.SemaphoreType.DMA
    small = 2 * cols + step_cols
    result, raw, retain, grown, vec = pl.pallas_call(
        lambda *refs: fused_kernel(tp, *refs),
        out_shape=(
            jax.ShapeDtypeStruct((rows, width), bf16),
            jax.ShapeDtypeStruct((layers, own, inner + 2 * cols), f32),
            jax.ShapeDtypeStruct((layers, own, inner), f32),
            jax.ShapeDtypeStruct((layers, own, inner), f32),
            jax.ShapeDtypeStruct((layers, own, state_dim), f32),
        ),
        in_specs=[vmem] * 8 + [hbm] * 7,
        out_specs=(vmem,) * 5,
        scratch_shapes=[
            pltpu.VMEM((layers, width, inner), bf16),
            pltpu.VMEM((layers, width, inner), bf16),
            pltpu.VMEM((layers, width, small), bf16),
            pltpu.VMEM((layers, inner, width), bf16),
            pltpu.VMEM((layers, own, heads, head_dim, state_dim), f32),
            pltpu.VMEM((tp * cols, state_dim), bf16),
            pltpu.VMEM((step_cols, inner), bf16),
            pltpu.VMEM((layers, rows, small + 128), f32),
            pltpu.VMEM((layers, rows, 2 * inner), f32),
            pltpu.VMEM((layers, own, small + 128), f32),
            pltpu.VMEM((layers, own, 2 * inner), f32),
            pltpu.VMEM((layers, tp, 2 * own, cols), bf16),
            pltpu.VMEM((layers, own, inner), f32),
            pltpu.VMEM((layers, own, inner), f32),
            pltpu.VMEM((layers, tp, rows, chunk), bf16),
            pltpu.VMEM((layers, tp, rows, chunk), bf16),
            pltpu.VMEM((layers, tp, rows, chunk), bf16),
            dma((7 * layers,)),
            dma((3 * layers,)),
            dma((3 * layers,)),
        ]
        + [dma((layers, tp))] * 6,
        compiler_params=pltpu.CompilerParams(
            collective_id=0, has_side_effects=True, vmem_limit_bytes=56 * 1024 * 1024
        ),
    )(
        hidden,
        norm_gain,
        taps[:, -1],
        pre,
        step_bias,
        decay_log,
        skip_gain,
        group_gain,
        gate_weight,
        inner_weight,
        write_weight,
        read_weight,
        step_weight,
        out_weight,
        recurrent,
    )
    fresh = raw.astype(jnp.bfloat16)[:, :, None, :]
    ends = (0, inner, inner + cols, inner + 2 * cols)
    nexts = [
        jnp.concatenate([state[:, :, 1:], fresh[..., a:b]], axis=2)
        for state, a, b in zip((state_inner, state_write, state_read), ends, ends[1:])
    ]
    split = (layers, own, heads, head_dim, 1)
    updated = (
        retain.reshape(split) * recurrent + grown.reshape(split) * vec[:, :, None, None, :]
    )
    return (result, nexts[0], nexts[1], nexts[2], updated)


def solution(mesh):
    tp = mesh.shape["tp"]
    fits = mesh.shape["dp"] == 2 and tp == GROUPS
    return jax.shard_map(
        fused_local if fits else local,
        mesh=mesh,
        in_specs=(
            P(None, "dp"),
            P(None, "dp"),
            P(None, "dp", "tp"),
            P(None, "dp", "tp"),
            P(None, "dp", "tp"),
            P(None, "dp", "tp"),
            P(None, "dp", None),
            P(None, None, "tp"),
            P(None, None, "tp"),
            P(None, None, "tp"),
            P(None, "tp"),
            P(None, "tp"),
            P(None, "tp"),
            P(None, "tp"),
            P(None, "tp", "dp"),
            P(None, "dp", None, "tp"),
            P(None, "dp", None, "tp"),
            P(None, "dp", None, "tp"),
            P(None, "dp", "tp", None, None),
        ),
        out_specs=(
            P(None, "dp"),
            P(None, "dp", None, "tp"),
            P(None, "dp", None, "tp"),
            P(None, "dp", None, "tp"),
            P(None, "dp", "tp", None, None),
        ),
        check_vma=False,
    )
```

```python
import jax
import jax.numpy as jnp
from jax import lax
from jax.experimental import pallas as pl
from jax.experimental.pallas import tpu as pltpu
from jax.sharding import PartitionSpec as P

D = 4096
HEADS = 128
GROUPS = 16


eps = 1e-06


def convolve(state, fresh_row, kernel):
    window = jnp.concatenate([state, fresh_row[:, None, :]], axis=1)
    summed = jnp.sum(window.astype(jnp.float32) * kernel.astype(jnp.float32)[None], axis=1)
    return (jax.nn.silu(summed), window[:, 1:])


def mixer_block(normed, number, weights):
    (
        gate_weight,
        inner_weight,
        write_weight,
        read_weight,
        step_weight,
        conv_inner,
        conv_write,
        conv_read,
        step_bias,
        decay_log,
        skip_gain,
        group_gain,
        out_weight,
        state_inner,
        state_write,
        state_read,
        recurrent,
    ) = weights

    def partial_of(weight):
        return jnp.dot(normed, weight[number], preferred_element_type=jnp.float32).astype(
            jnp.bfloat16
        )

    summed = (
        lax.psum_scatter(partial_of(gate_weight), "dp", scatter_dimension=0, tiled=True).astype(
            jnp.float32
        ),
        lax.psum_scatter(partial_of(inner_weight), "dp", scatter_dimension=0, tiled=True).astype(
            jnp.float32
        ),
        lax.psum_scatter(partial_of(write_weight), "dp", scatter_dimension=0, tiled=True).astype(
            jnp.float32
        ),
        lax.psum_scatter(partial_of(read_weight), "dp", scatter_dimension=0, tiled=True).astype(
            jnp.float32
        ),
        lax.psum_scatter(partial_of(step_weight), "dp", scatter_dimension=0, tiled=True).astype(
            jnp.float32
        ),
    )
    gate_raw, inner_raw, write_raw, read_raw, step_raw = [
        member.astype(jnp.bfloat16) for member in summed
    ]
    inner_act, next_inner = convolve(state_inner[number], inner_raw, conv_inner[number])
    write_act, next_write = convolve(state_write[number], write_raw, conv_write[number])
    read_act, next_read = convolve(state_read[number], read_raw, conv_read[number])
    write_all, read_all = (
        lax.all_gather(write_act.astype(jnp.bfloat16), "tp", axis=1, tiled=True),
        lax.all_gather(read_act.astype(jnp.bfloat16), "tp", axis=1, tiled=True),
    )
    heads_here = step_bias.shape[1]
    head_dim = recurrent.shape[3]
    state_dim = recurrent.shape[4]
    rows_here = inner_act.shape[0]
    first_head = lax.axis_index("tp") * heads_here
    group_index = first_head // (HEADS // GROUPS)
    write_grid = write_all.reshape(rows_here, state_dim, GROUPS)
    read_grid = read_all.reshape(rows_here, state_dim, GROUPS)
    write_vec = lax.dynamic_slice_in_dim(write_grid, group_index, 1, 2)[:, :, 0].astype(jnp.float32)
    read_vec = lax.dynamic_slice_in_dim(read_grid, group_index, 1, 2)[:, :, 0].astype(jnp.float32)
    step_own = lax.dynamic_slice_in_dim(step_raw, first_head, heads_here, 1)
    step_size = jax.nn.softplus(step_own.astype(jnp.float32) + step_bias[number][None, :])
    retain = jnp.exp(-step_size * jnp.exp(decay_log[number])[None, :])
    inner_heads = inner_act.reshape(rows_here, heads_here, head_dim)
    updated = (
        retain[:, :, None, None] * recurrent[number]
        + (step_size[:, :, None] * inner_heads)[:, :, :, None] * write_vec[:, None, None, :]
    )
    readout = jnp.einsum("bhpn,bn->bhp", updated, read_vec, precision=lax.Precision.HIGHEST)
    readout = readout + skip_gain[number][None, :, None] * inner_heads
    gated_out = readout.reshape(rows_here, heads_here * head_dim) * jax.nn.silu(
        gate_raw.astype(jnp.float32)
    )
    selector = (jnp.arange(GROUPS) == group_index).astype(jnp.float32)
    totals = lax.psum(jnp.sum(gated_out * gated_out, axis=1)[:, None] * selector[None, :], "tp")
    group_sum = jnp.sum(totals * selector[None, :], axis=1, keepdims=True)
    group_factor = lax.rsqrt(group_sum / (HEADS // GROUPS * head_dim) + eps)
    group_normed = (gated_out * group_factor * group_gain[number][None, :]).astype(jnp.bfloat16)
    branch = jnp.dot(
        lax.all_gather(group_normed, "dp", axis=0, tiled=True),
        out_weight[number],
        preferred_element_type=jnp.float32,
    )
    return (branch, (next_inner, next_write, next_read, updated))


def total_over(branch):
    return lax.psum(branch, "tp")


def local(
    hidden,
    norm_gain,
    gate_weight,
    inner_weight,
    write_weight,
    read_weight,
    step_weight,
    conv_inner,
    conv_write,
    conv_read,
    step_bias,
    decay_log,
    skip_gain,
    group_gain,
    out_weight,
    state_inner,
    state_write,
    state_read,
    recurrent,
):
    weights = (
        gate_weight,
        inner_weight,
        write_weight,
        read_weight,
        step_weight,
        conv_inner,
        conv_write,
        conv_read,
        step_bias,
        decay_log,
        skip_gain,
        group_gain,
        out_weight,
        state_inner,
        state_write,
        state_read,
        recurrent,
    )
    wide_in = hidden.astype(jnp.float32)
    squares = lax.psum(jnp.sum(wide_in * wide_in, axis=1, keepdims=True), "dp")
    normed = (wide_in * lax.rsqrt(squares / D + eps) * norm_gain[0][None, :]).astype(jnp.bfloat16)
    branch, first_states = mixer_block(normed, 0, weights)
    middle = (wide_in + total_over(branch)).astype(jnp.bfloat16).astype(jnp.float32)
    squares = lax.psum(jnp.sum(middle * middle, axis=1, keepdims=True), "dp")
    normed = (middle * lax.rsqrt(squares / D + eps) * norm_gain[1][None, :]).astype(jnp.bfloat16)
    branch, second_states = mixer_block(normed, 1, weights)
    result = (middle + total_over(branch)).astype(jnp.bfloat16)
    stacked = [jnp.stack([earlier, later]) for earlier, later in zip(first_states, second_states)]
    return (result, stacked[0], stacked[1], stacked[2], stacked[3])


def fused_kernel(
    tp,
    hidden_ref,
    norm_gain_ref,
    conv_i_ref,
    conv_w_ref,
    conv_r_ref,
    state_i_ref,
    state_w_ref,
    state_r_ref,
    bias_ref,
    decay_ref,
    skip_ref,
    group_gain_ref,
    gate_hbm,
    inner_hbm,
    write_hbm,
    read_hbm,
    step_hbm,
    out_hbm,
    rec_hbm,
    result_ref,
    fresh_i_ref,
    fresh_w_ref,
    fresh_r_ref,
    updated_hbm,
    gate_v,
    inner_v,
    small_v,
    out_v,
    rec_v,
    pick_v,
    spread_v,
    part_a,
    part_b,
    got_a,
    got_b,
    gath,
    normed_mine,
    normed_peer,
    branch_v,
    red,
    stream_v,
    turned_v,
    w_sem,
    u_sem,
    dp_send,
    dp_recv,
    gath_send,
    gath_recv,
    red_send,
    red_recv,
    str_send,
    str_recv,
):
    t = lax.axis_index("tp")
    me = lax.axis_index("dp")
    peer = 1 - me
    layers = norm_gain_ref.shape[0]
    rows = hidden_ref.shape[0]
    own = rows // 2
    width = hidden_ref.shape[1]
    total_width = width * 2
    inner = gate_hbm.shape[2]
    cols = write_hbm.shape[2]
    step_cols = step_hbm.shape[2]
    small = 2 * cols + step_cols
    chunk = width // tp
    heads = bias_ref.shape[1]
    head_dim = inner // heads

    def load(source, target, number):
        return pltpu.make_async_copy(source, target, w_sem.at[number])

    loads = []
    for l in range(layers):
        at = 7 * l
        loads.append(
            [
                load(write_hbm.at[l], small_v.at[l, :, pl.ds(0, cols)], at),
                load(read_hbm.at[l], small_v.at[l, :, pl.ds(cols, cols)], at + 1),
                load(step_hbm.at[l], small_v.at[l, :, pl.ds(2 * cols, step_cols)], at + 2),
                load(inner_hbm.at[l], inner_v.at[l], at + 3),
                load(gate_hbm.at[l], gate_v.at[l], at + 4),
                load(rec_hbm.at[l], rec_v.at[l], at + 5),
                load(out_hbm.at[l], out_v.at[l], at + 6),
            ]
        )
    for one in loads[0]:
        one.start()

    barrier = pltpu.get_barrier_semaphore()

    @pl.loop(1, tp)
    def _(k):
        pl.semaphore_signal(barrier, inc=1, device_id={"tp": lax.rem(t + k, tp), "dp": me})

    pl.semaphore_signal(barrier, inc=1, device_id={"tp": t, "dp": peer})

    big = pick_v.shape
    pick_v[...] = (
        lax.broadcasted_iota(jnp.int32, big, 0)
        == lax.broadcasted_iota(jnp.int32, big, 1) * tp + t
    ).astype(jnp.float32).astype(jnp.bfloat16)
    grid = spread_v.shape
    lane_head = lax.broadcasted_iota(jnp.int32, grid, 1) // head_dim
    spread_v[...] = (
        lax.broadcasted_iota(jnp.int32, grid, 0) == lane_head + heads * t
    ).astype(jnp.float32).astype(jnp.bfloat16)

    wide_head = lax.broadcasted_iota(jnp.int32, (own, inner), 1) // head_dim
    own_row = lax.broadcasted_iota(jnp.int32, (own, inner), 0)

    def widen(row):
        wide = jnp.zeros((own, inner), jnp.float32)
        for h in range(heads):
            wide = jnp.where(
                wide_head == h, jnp.broadcast_to(row[:, h : h + 1], (own, inner)), wide
            )
        return wide

    bias_w = [widen(bias_ref[l : l + 1, :]) for l in range(layers)]
    rate_w = [widen(jnp.exp(decay_ref[l : l + 1, :])) for l in range(layers)]
    skip_w = [widen(skip_ref[l : l + 1, :]) for l in range(layers)]

    def to_peer(source, target, number):
        return pltpu.make_async_remote_copy(
            src_ref=source,
            dst_ref=target,
            send_sem=dp_send.at[number],
            recv_sem=dp_recv.at[number],
            device_id={"tp": t, "dp": peer},
        )

    def earlier_taps(state_ref, conv_ref, l):
        taps = conv_ref[l].astype(jnp.float32)
        count = state_ref.shape[1]
        total = state_ref[l, 0].astype(jnp.float32) * taps[0:1]
        for k in range(1, count):
            total = total + state_ref[l, k].astype(jnp.float32) * taps[k : k + 1]
        return total, taps[count : count + 1]

    def spread_start(source_of, target, sends, recvs):
        @pl.loop(1, tp)
        def _(k):
            to = lax.rem(t + k, tp)
            pltpu.make_async_remote_copy(
                src_ref=source_of(to),
                dst_ref=target.at[t],
                send_sem=sends.at[to],
                recv_sem=recvs.at[t],
                device_id={"tp": to, "dp": me},
            ).start()

    def spread_wait(source_of, target, sends, recvs):
        @pl.loop(1, tp)
        def _(k):
            to = lax.rem(t + k, tp)
            copy = pltpu.make_async_remote_copy(
                src_ref=source_of(to),
                dst_ref=target.at[to],
                send_sem=sends.at[to],
                recv_sem=recvs.at[to],
                device_id={"tp": to, "dp": me},
            )
            copy.wait_send()
            copy.wait_recv()

    first = True
    mine = pl.ds(pl.multiple_of(me * own, own), own)
    theirs = pl.ds(pl.multiple_of(peer * own, own), own)
    wide = hidden_ref[...].astype(jnp.float32)
    for l in range(layers):
        scaled = (wide * norm_gain_ref[l : l + 1, :]).astype(jnp.bfloat16)
        squares = jnp.sum(wide * wide, axis=1, keepdims=True)
        for one in loads[l][:3]:
            one.wait()
        part_a[l, :, 0:small] = jnp.dot(scaled, small_v[l], preferred_element_type=jnp.float32)
        part_a[l, :, small : small + 128] = jnp.broadcast_to(squares, (rows, 128))
        if first:
            pl.semaphore_wait(barrier, tp)
            first = False
        send_a = to_peer(part_a.at[l, theirs], got_a.at[l], 3 * l)
        send_a.start()
        if l + 1 < layers:
            for one in loads[l + 1]:
                one.start()
        loads[l][3].wait()
        part_b[l, :, 0:inner] = jnp.dot(scaled, inner_v[l], preferred_element_type=jnp.float32)
        loads[l][4].wait()
        part_b[l, :, inner : 2 * inner] = jnp.dot(
            scaled, gate_v[l], preferred_element_type=jnp.float32
        )
        send_b = to_peer(part_b.at[l, theirs], got_b.at[l], 3 * l + 1)
        send_b.start()
        pre_w = earlier_taps(state_w_ref, conv_w_ref, l)
        pre_r = earlier_taps(state_r_ref, conv_r_ref, l)
        pre_i = earlier_taps(state_i_ref, conv_i_ref, l)
        send_a.wait()
        sum_a = part_a[l, mine, :] + got_a[l]
        factor = lax.rsqrt(sum_a[:, small : small + 1] / total_width + eps)
        raw_a = (sum_a[:, 0:small] * factor).astype(jnp.bfloat16).astype(jnp.float32)
        acts = []
        for fresh_ref, (early, tap), raw in (
            (fresh_w_ref, pre_w, raw_a[:, 0:cols]),
            (fresh_r_ref, pre_r, raw_a[:, cols : 2 * cols]),
        ):
            fresh_ref[l] = raw.astype(jnp.bfloat16)
            tapped = early + raw * tap
            acts.append(tapped * jax.nn.sigmoid(tapped))
        gath[l, t] = jnp.concatenate(acts, axis=0).astype(jnp.bfloat16)
        spread_start(lambda to: gath.at[l, t], gath.at[l], gath_send.at[l], gath_recv.at[l])
        step_raw = raw_a[:, 2 * cols :]
        step = (
            jnp.dot(
                jnp.concatenate([step_raw, step_raw], axis=0).astype(jnp.bfloat16),
                spread_v[...],
                preferred_element_type=jnp.float32,
            )[:own]
            + bias_w[l]
        )
        step = jnp.maximum(step, 0.0) + jnp.log1p(jnp.exp(-jnp.abs(step)))
        retain = jnp.exp(-step * rate_w[l])
        send_b.wait()
        raw_b = (
            ((part_b[l, mine, :] + got_b[l]) * factor).astype(jnp.bfloat16).astype(jnp.float32)
        )
        fresh_i_ref[l] = raw_b[:, 0:inner].astype(jnp.bfloat16)
        act = pre_i[0] + raw_b[:, 0:inner] * pre_i[1]
        act = act * jax.nn.sigmoid(act)
        gate = raw_b[:, inner:]
        gate = gate * jax.nn.sigmoid(gate)
        grown = step * act
        loads[l][5].wait()
        for b in range(own):
            turned_v[b] = rec_v[l, b].reshape(inner, rec_v.shape[-1]).T.astype(jnp.bfloat16)
        spread_wait(lambda to: gath.at[l, t], gath.at[l], gath_send.at[l], gath_recv.at[l])
        both = jnp.dot(
            jnp.concatenate([gath[l, k] for k in range(tp)], axis=1),
            pick_v[...],
            preferred_element_type=jnp.float32,
        )
        overlap = jnp.sum(both[:own] * both[own:], axis=1, keepdims=True)
        low = both.astype(jnp.bfloat16)
        carried = jnp.zeros((own, inner), jnp.float32)
        for b in range(own):
            row = jnp.dot(low, turned_v[b], preferred_element_type=jnp.float32)
            carried = jnp.where(own_row == b, row[own:], carried)
        gated = (retain * carried + grown * overlap + skip_w[l] * act) * gate
        group = jnp.sum(gated * gated, axis=1, keepdims=True) / inner
        normed = gated * lax.rsqrt(group + eps) * group_gain_ref[l : l + 1, :]
        normed_mine[l] = normed
        send_c = to_peer(normed_mine.at[l], normed_peer.at[l], 3 * l + 2)
        send_c.start()
        loads[l][6].wait()
        send_c.wait()
        other = normed_peer[l]
        lower = me == 0
        left = jnp.concatenate(
            [jnp.where(lower, normed, other), jnp.where(lower, other, normed)], axis=0
        ).astype(jnp.bfloat16)
        branch = jnp.dot(left, out_v[l], preferred_element_type=jnp.float32).astype(jnp.bfloat16)
        for k in range(tp):
            branch_v[l, k] = branch[:, k * chunk : (k + 1) * chunk]
        spread_start(lambda to: branch_v.at[l, to], red.at[l], red_send.at[l], red_recv.at[l])
        red[l, t] = branch_v[l, t]
        turned = jnp.concatenate([retain, grown], axis=0).T
        for b in range(own):
            state = rec_v[l, b].reshape(inner, rec_v.shape[-1])
            state = turned[:, b : b + 1] * state + turned[:, own + b : own + b + 1] * both[b : b + 1]
            rec_v[l, b] = state.reshape(rec_v.shape[2:])
        pltpu.make_async_copy(rec_v.at[l], updated_hbm.at[l], u_sem.at[l]).start()
        spread_wait(lambda to: branch_v.at[l, to], red.at[l], red_send.at[l], red_recv.at[l])
        total = red[l, 0].astype(jnp.float32)
        for k in range(1, tp):
            total = total + red[l, k].astype(jnp.float32)
        if l == 0:
            before = hidden_ref[:, pl.ds(pl.multiple_of(t * chunk, chunk), chunk)]
        else:
            before = stream_v[l - 1, t]
        stream_v[l, t] = (total + before.astype(jnp.float32)).astype(jnp.bfloat16)
        spread_start(lambda to: stream_v.at[l, t], stream_v.at[l], str_send.at[l], str_recv.at[l])
        spread_wait(lambda to: stream_v.at[l, t], stream_v.at[l], str_send.at[l], str_recv.at[l])
        after = jnp.concatenate([stream_v[l, k] for k in range(tp)], axis=1)
        if l == layers - 1:
            result_ref[...] = after
        else:
            wide = after.astype(jnp.float32)
    for l in range(layers):
        pltpu.make_async_copy(rec_v.at[l], updated_hbm.at[l], u_sem.at[l]).wait()


def fused_local(
    hidden,
    norm_gain,
    gate_weight,
    inner_weight,
    write_weight,
    read_weight,
    step_weight,
    conv_inner,
    conv_write,
    conv_read,
    step_bias,
    decay_log,
    skip_gain,
    group_gain,
    out_weight,
    state_inner,
    state_write,
    state_read,
    recurrent,
):
    tp = lax.axis_size("tp")
    layers, width, inner = gate_weight.shape
    cols = write_weight.shape[2]
    step_cols = step_weight.shape[2]
    rows = hidden.shape[0]
    own, heads, head_dim, state_dim = recurrent.shape[1:]
    chunk = width // tp
    vmem = pl.BlockSpec(memory_space=pltpu.VMEM)
    hbm = pl.BlockSpec(memory_space=pl.ANY)
    f32, bf16 = jnp.float32, jnp.bfloat16
    dma = pltpu.SemaphoreType.DMA
    small = 2 * cols + step_cols
    result, *fresh, updated = pl.pallas_call(
        lambda *refs: fused_kernel(tp, *refs),
        out_shape=(
            jax.ShapeDtypeStruct((rows, width), bf16),
            jax.ShapeDtypeStruct((layers, own, inner), bf16),
            jax.ShapeDtypeStruct((layers, own, cols), bf16),
            jax.ShapeDtypeStruct((layers, own, cols), bf16),
            jax.ShapeDtypeStruct(recurrent.shape, f32),
        ),
        in_specs=[vmem] * 12 + [hbm] * 7,
        out_specs=(vmem,) * 4 + (hbm,),
        scratch_shapes=[
            pltpu.VMEM((layers, width, inner), bf16),
            pltpu.VMEM((layers, width, inner), bf16),
            pltpu.VMEM((layers, width, small), bf16),
            pltpu.VMEM((layers, inner, width), bf16),
            pltpu.VMEM((layers, own, heads, head_dim, state_dim), f32),
            pltpu.VMEM((tp * cols, state_dim), bf16),
            pltpu.VMEM((step_cols, inner), bf16),
            pltpu.VMEM((layers, rows, small + 128), f32),
            pltpu.VMEM((layers, rows, 2 * inner), f32),
            pltpu.VMEM((layers, own, small + 128), f32),
            pltpu.VMEM((layers, own, 2 * inner), f32),
            pltpu.VMEM((layers, tp, 2 * own, cols), bf16),
            pltpu.VMEM((layers, own, inner), f32),
            pltpu.VMEM((layers, own, inner), f32),
            pltpu.VMEM((layers, tp, rows, chunk), bf16),
            pltpu.VMEM((layers, tp, rows, chunk), bf16),
            pltpu.VMEM((layers, tp, rows, chunk), bf16),
            pltpu.VMEM((own, state_dim, inner), bf16),
            dma((7 * layers,)),
            dma((layers,)),
            dma((3 * layers,)),
            dma((3 * layers,)),
        ]
        + [dma((layers, tp))] * 6,
        compiler_params=pltpu.CompilerParams(
            collective_id=0, has_side_effects=True, vmem_limit_bytes=56 * 1024 * 1024
        ),
    )(
        hidden,
        norm_gain,
        conv_inner,
        conv_write,
        conv_read,
        jnp.swapaxes(state_inner, 1, 2),
        jnp.swapaxes(state_write, 1, 2),
        jnp.swapaxes(state_read, 1, 2),
        step_bias,
        decay_log,
        skip_gain,
        group_gain,
        gate_weight,
        inner_weight,
        write_weight,
        read_weight,
        step_weight,
        out_weight,
        recurrent,
    )
    nexts = [
        jnp.concatenate([state[:, :, 1:], new[:, :, None]], axis=2)
        for state, new in zip((state_inner, state_write, state_read), fresh)
    ]
    return (result, nexts[0], nexts[1], nexts[2], updated)


def solution(mesh):
    tp = mesh.shape["tp"]
    fits = mesh.shape["dp"] == 2 and tp == GROUPS
    return jax.shard_map(
        fused_local if fits else local,
        mesh=mesh,
        in_specs=(
            P(None, "dp"),
            P(None, "dp"),
            P(None, "dp", "tp"),
            P(None, "dp", "tp"),
            P(None, "dp", "tp"),
            P(None, "dp", "tp"),
            P(None, "dp", None),
            P(None, None, "tp"),
            P(None, None, "tp"),
            P(None, None, "tp"),
            P(None, "tp"),
            P(None, "tp"),
            P(None, "tp"),
            P(None, "tp"),
            P(None, "tp", "dp"),
            P(None, "dp", None, "tp"),
            P(None, "dp", None, "tp"),
            P(None, "dp", None, "tp"),
            P(None, "dp", "tp", None, None),
        ),
        out_specs=(
            P(None, "dp"),
            P(None, "dp", None, "tp"),
            P(None, "dp", None, "tp"),
            P(None, "dp", None, "tp"),
            P(None, "dp", "tp", None, None),
        ),
        check_vma=False,
    )
```
